32 devices in a mesh: ra: 4 (over z), cb: 4 (over y, x), dp: 2 (over core).
Axes of the slice: x: 2, y: 2, z: 4, core: 2. Of those that a mesh axis runs over, the one named last changes fastest.
Arguments:
- tokens: bfloat16 [256, 4096], P('dp', 'ra'), may hold values from -24 to 24
- first_gain: float32 [4096], P('ra'), may hold values from 0.1 to 1.9
- first_gate: float32 [4096, 11264], P('ra', 'cb'), may hold values from -0.125 to 0.125
- first_gate_scale: float32 [11264], P('cb'), may hold values from 0.5 to 2
- first_up: float32 [4096, 11264], P('ra', 'cb'), may hold values from -0.125 to 0.125
- first_up_scale: float32 [11264], P('cb'), may hold values from 0.5 to 2
- first_down: float32 [11264, 4096], P('cb', 'ra'), may hold values from -0.0546875 to 0.0546875
- first_down_scale: float32 [4096], P('ra'), may hold values from 0.5 to 2
- second_gain: float32 [4096], P('ra'), may hold values from 0.1 to 1.9
- second_gate: float32 [4096, 11264], P('ra', 'cb'), may hold values from -0.125 to 0.125
- second_gate_scale: float32 [11264], P('cb'), may hold values from 0.5 to 2
- second_up: float32 [4096, 11264], P('ra', 'cb'), may hold values from -0.125 to 0.125
- second_up_scale: float32 [11264], P('cb'), may hold values from 0.5 to 2
- second_down: float32 [11264, 4096], P('cb', 'ra'), may hold values from -0.0546875 to 0.0546875
- second_down_scale: float32 [4096], P('ra'), may hold values from 0.5 to 2
Outputs:
- mixed: float32 [256, 4096], P('dp', 'ra')
The draws below stay inside these ranges and needn't reach their ends.
All inputs are finite; a program needn't handle non-finite values.
Results may differ from the reference program's by a relative error of at most 0.0083.
Values may be sent and summed in bfloat16 or wider, within the bound.
A program may use at most 128 MiB of HBM per device.

```python
import math
import jax
import jax.numpy as jnp
from jax import lax

D = 4096
FF = 11264
TOKENS = 256


def draw_tokens(key, part):
    first, second, third = jax.random.split(key, 3)
    values = jax.random.normal(first, (TOKENS, D), jnp.float32)
    blocks = jnp.exp(jax.random.uniform(second, (32,), jnp.float32, -1.2, 1.2))
    columns = jnp.repeat(blocks, D // 32)
    rows = jnp.exp(jax.random.uniform(third, (TOKENS, 1), jnp.float32, -0.7, 0.7))
    values = values * rows
    return jnp.clip(values * columns, -24.0, 24.0).astype(jnp.bfloat16)


def strengthened(drawn, rng, source, target, blocks, factor):
    owner, partner = [(jnp.arange(drawn.shape[dim]) // (drawn.shape[dim] // blocks)).reshape([-1 if axis == dim else 1 for axis in range(drawn.ndim)]) for dim in (source, target)]
    chosen = jax.random.permutation(rng, blocks)[partner]
    strong = (owner == chosen) | (owner == (partner + blocks // 2) % blocks)
    return jnp.where(strong, factor * drawn, drawn)


def block_scale(own_key, shape, cuts, least, top_value):
    def one(position, shards_of):
        draws = jax.random.uniform(jax.random.fold_in(jax.random.fold_in(own_key, 6), position), (shards_of,), jnp.float32, least / len(cuts), top_value / len(cuts))
        return jnp.repeat(jnp.exp(draws), shape[position] // shards_of).reshape((-1,) + (1,) * (len(shape) - position - 1))

    level = one(*cuts[0])
    for cut in cuts[1:]:
        level = level * one(*cut)
    return level


def scatter_about(own_key, shape, spread, most, cuts=(), held_as=jnp.bfloat16):
    result = jax.random.normal(own_key, shape, jnp.float32) * spread
    if len(cuts) > 0:
        result = block_scale(own_key, shape, cuts, -0.22, 0.18) * result
    return jnp.clip(result, min=-most, max=most).astype(held_as)


def noise_with(stream_key, extent, deviation, most, shards, heavy, kind=jnp.bfloat16):
    drawn = deviation * jax.random.normal(stream_key, extent, jnp.float32)
    if shards:
        drawn = drawn * block_scale(stream_key, extent, shards, -0.22, 0.18)
    return jnp.clip(strengthened(drawn, jax.random.fold_in(stream_key, 3), *heavy), -most, most).astype(kind)


def setup_inputs(seed: int = 0) -> dict:
    seeds = jax.random.split(jax.random.key(seed), 16)
    tokens = draw_tokens(jax.random.fold_in(seeds[15], 71), 0)
    first_gain = jnp.clip(1.0 + 0.18 * jax.random.normal(seeds[1], (D,), jnp.float32), 0.1, 1.9)
    first_gate = noise_with(seeds[2], (D, FF), D ** -0.5, 0.125, ((0, 4), (1, 4)), (0, 1, 4, 2.0), jnp.float32)
    first_gate_scale = jnp.clip(jnp.exp(math.log(2.0) - 1.3862944 * jax.random.uniform(seeds[3], (FF,), jnp.float32) ** block_scale(seeds[3], (FF,), ((0, 4),), -0.2, 0.2)), 0.5, 2.0)
    first_up = noise_with(seeds[4], (D, FF), D ** -0.5, 0.125, ((0, 4), (1, 4)), (0, 1, 4, 2.0), jnp.float32)
    first_up_scale = jnp.clip(jnp.exp(math.log(2.0) - 1.3862944 * jax.random.uniform(seeds[5], (FF,), jnp.float32) ** block_scale(seeds[5], (FF,), ((0, 4),), -0.2, 0.2)), 0.5, 2.0)
    first_down = scatter_about(seeds[6], (FF, D), FF ** -0.5, 0.0546875, ((0, 4), (1, 4)), jnp.float32)
    first_down_scale = jnp.clip(jnp.exp(math.log(2.0) - 1.3862944 * jax.random.uniform(seeds[7], (D,), jnp.float32) ** block_scale(seeds[7], (D,), ((0, 4),), -0.2, 0.2)), 0.5, 2.0)
    second_gain = jnp.clip(1.0 + 0.18 * jax.random.normal(seeds[8], (D,), jnp.float32), 0.1, 1.9)
    second_gate = noise_with(seeds[9], (D, FF), D ** -0.5, 0.125, ((0, 4), (1, 4)), (0, 1, 4, 2.0), jnp.float32)
    second_gate_scale = jnp.clip(jnp.exp(math.log(2.0) - 1.3862944 * jax.random.uniform(seeds[10], (FF,), jnp.float32) ** block_scale(seeds[10], (FF,), ((0, 4),), -0.2, 0.2)), 0.5, 2.0)
    second_up = noise_with(seeds[11], (D, FF), D ** -0.5, 0.125, ((0, 4), (1, 4)), (0, 1, 4, 2.0), jnp.float32)
    second_up_scale = jnp.clip(jnp.exp(math.log(2.0) - 1.3862944 * jax.random.uniform(seeds[12], (FF,), jnp.float32) ** block_scale(seeds[12], (FF,), ((0, 4),), -0.2, 0.2)), 0.5, 2.0)
    second_down = scatter_about(seeds[13], (FF, D), FF ** -0.5, 0.0546875, ((0, 4), (1, 4)), jnp.float32)
    second_down_scale = jnp.clip(jnp.exp(math.log(2.0) - 1.3862944 * jax.random.uniform(seeds[14], (D,), jnp.float32) ** block_scale(seeds[14], (D,), ((0, 4),), -0.2, 0.2)), 0.5, 2.0)
    return dict(tokens=tokens, first_gain=first_gain, first_gate=first_gate, first_gate_scale=first_gate_scale, first_up=first_up, first_up_scale=first_up_scale, first_down=first_down, first_down_scale=first_down_scale, second_gain=second_gain, second_gate=second_gate, second_gate_scale=second_gate_scale, second_up=second_up, second_up_scale=second_up_scale, second_down=second_down, second_down_scale=second_down_scale)


def half_step(stream, gain, gate_w, gate_scale, up_w, up_scale, down_w, down_scale):
    inverse = lax.rsqrt(lax.optimization_barrier(jnp.mean(stream * stream, axis=1, keepdims=True)) + 1e-06)
    scaled = (stream * gain).astype(jnp.bfloat16)
    gate = jnp.dot(scaled, gate_w.astype(jnp.bfloat16), preferred_element_type=jnp.float32) * inverse * gate_scale
    up = jnp.dot(scaled, up_w.astype(jnp.bfloat16), preferred_element_type=jnp.float32) * inverse * up_scale
    hidden = (jax.nn.silu(gate) * up).astype(jnp.bfloat16)
    branch = jnp.dot(hidden, down_w.astype(jnp.bfloat16), preferred_element_type=jnp.float32) * down_scale
    return 0.5 * stream + 0.5 * branch

def reference(tokens, first_gain, first_gate, first_gate_scale, first_up, first_up_scale, first_down, first_down_scale, second_gain, second_gate, second_gate_scale, second_up, second_up_scale, second_down, second_down_scale):
    stream = tokens.astype(jnp.float32)
    stream = half_step(stream, first_gain, first_gate, first_gate_scale, first_up, first_up_scale, first_down, first_down_scale)
    stream = half_step(stream, second_gain, second_gate, second_gate_scale, second_up, second_up_scale, second_down, second_down_scale)
    return stream
```

```python
import functools

import jax
import jax.numpy as jnp
from jax import lax
from jax.experimental import pallas as pl
from jax.experimental.pallas import tpu as pltpu
from jax.sharding import PartitionSpec as P

MESH = pl.DeviceIdType.MESH
F32 = jnp.float32
BF16 = jnp.bfloat16


def chunk_of(total):
    for size in (256, 128):
        if total % size == 0:
            return size
    return total


def kernel(
    nra,
    ncb,
    width,
    tokens_ref,
    gain1_ref,
    gscale1_ref,
    uscale1_ref,
    dscale1_ref,
    gain2_ref,
    gscale2_ref,
    uscale2_ref,
    dscale2_ref,
    gate1_hbm,
    up1_hbm,
    down1_hbm,
    gate2_hbm,
    up2_hbm,
    down2_hbm,
    out_ref,
    wg,
    wu,
    wd,
    stream,
    scaled,
    acc,
    squares,
    squares_in,
    part,
    part_in,
    hid,
    branch_part,
    branch_in,
    branch,
    wg_sem,
    wu_sem,
    wd_sem,
    part_send,
    part_recv,
    hid_send,
    hid_recv,
    small_send,
    small_recv,
):
    ra = lax.axis_index("ra")
    cb = lax.axis_index("cb")
    chunks, depth, size = wg.shape
    tokens = stream.shape[0]
    rows = tokens // nra
    crow = tokens // ncb

    def columns(c):
        return pl.ds(pl.multiple_of(c * size, size), size)

    def load_in(gate_hbm, up_hbm, c):
        return (
            pltpu.make_async_copy(gate_hbm.at[:, columns(c)], wg.at[c], wg_sem.at[c]),
            pltpu.make_async_copy(up_hbm.at[:, columns(c)], wu.at[c], wu_sem.at[c]),
        )

    def load_down(down_hbm, c):
        return pltpu.make_async_copy(down_hbm.at[columns(c), :], wd.at[c], wd_sem.at[c])

    def ra_peer(d):
        return lax.rem(ra + d, nra)

    def cb_peer(d):
        return lax.rem(cb + d, ncb)

    def wait_bytes(ref, sem):
        pltpu.make_async_copy(ref, ref, sem).wait()

    @pl.loop(0, chunks)
    def _(c):
        for copy in load_in(gate1_hbm, up1_hbm, c):
            copy.start()

    @pl.loop(0, chunks)
    def _(c):
        load_down(down1_hbm, c).start()

    barrier = pltpu.get_barrier_semaphore()
    for d in range(1, nra):
        pl.semaphore_signal(barrier, inc=1, device_id={"ra": ra_peer(d)}, device_id_type=MESH)
    for d in range(1, ncb):
        pl.semaphore_signal(barrier, inc=1, device_id={"cb": cb_peer(d)}, device_id_type=MESH)

    stream[...] = tokens_ref[...].astype(F32)
    pl.semaphore_wait(barrier, nra + ncb - 2)

    halves = (
        (gain1_ref, gscale1_ref, uscale1_ref, dscale1_ref, gate1_hbm, up1_hbm, down1_hbm),
        (gain2_ref, gscale2_ref, uscale2_ref, dscale2_ref, gate2_hbm, up2_hbm, down2_hbm),
    )
    for half in range(2):
        gain_ref, gscale_ref, uscale_ref, dscale_ref, gate_hbm, up_hbm, down_hbm = halves[half]
        value = stream[...]
        scaled[...] = (value * gain_ref[...]).astype(BF16)
        sums = jnp.sum(value * value, axis=1, keepdims=True)
        squares[...] = jnp.broadcast_to(sums, (tokens, 128)).reshape(nra, rows, 128)
        for d in range(1, nra):
            pltpu.make_async_remote_copy(
                src_ref=squares.at[ra_peer(d)],
                dst_ref=squares_in.at[d - 1],
                send_sem=small_send.at[0],
                recv_sem=small_recv.at[0],
                device_id={"ra": ra_peer(d)},
                device_id_type=MESH,
            ).start()

        @pl.loop(0, chunks)
        def _(c):
            for copy in load_in(gate_hbm, up_hbm, c):
                copy.wait()
            lhs = scaled[...]
            gate = jnp.dot(lhs, wg[c].astype(BF16), preferred_element_type=F32)
            up = jnp.dot(lhs, wu[c].astype(BF16), preferred_element_type=F32)
            part[c, :, :, :size] = gate.astype(BF16).reshape(nra, rows, size)
            part[c, :, :, size:] = up.astype(BF16).reshape(nra, rows, size)
            for d in range(1, nra):
                pltpu.make_async_remote_copy(
                    src_ref=part.at[c, ra_peer(d)],
                    dst_ref=part_in.at[c, d - 1],
                    send_sem=part_send.at[c],
                    recv_sem=part_recv.at[c],
                    device_id={"ra": ra_peer(d)},
                    device_id_type=MESH,
                ).start()
            if half == 0:
                for copy in load_in(gate2_hbm, up2_hbm, c):
                    copy.start()

        wait_bytes(squares_in, small_recv.at[0])
        total = squares[ra]
        for d in range(1, nra):
            total = total + squares_in[d - 1]
        squares_in[0] = lax.rsqrt(total / width + 1e-06)

        @pl.loop(0, chunks)
        def _(c):
            wait_bytes(part_in.at[c], part_recv.at[c])
            both = part[c, ra].astype(F32)
            for d in range(1, nra):
                both = both + part_in[c, d - 1].astype(F32)
            inverse = squares_in[0][:, :1]
            gate = both[:, :size] * inverse * gscale_ref[:, columns(c)]
            up = both[:, size:] * inverse * uscale_ref[:, columns(c)]
            hid[c, ra] = (gate / (1.0 + jnp.exp(-gate)) * up).astype(BF16)
            for d in range(1, nra):
                pltpu.make_async_remote_copy(
                    src_ref=hid.at[c, ra],
                    dst_ref=hid.at[c, ra],
                    send_sem=hid_send.at[c],
                    recv_sem=hid_recv.at[c],
                    device_id={"ra": ra_peer(d)},
                    device_id_type=MESH,
                ).start()

        acc[...] = jnp.zeros_like(acc)

        @pl.loop(0, chunks)
        def _(c):
            wait_bytes(hid.at[c, pl.ds(0, nra - 1)], hid_recv.at[c])
            load_down(down_hbm, c).wait()
            acc[...] += jnp.dot(
                hid[c].reshape(tokens, size), wd[c].astype(BF16), preferred_element_type=F32
            )
            if half == 0:
                load_down(down2_hbm, c).start()

        branch_part[...] = acc[...].astype(BF16).reshape(branch_part.shape)
        for d in range(1, ncb):
            pltpu.make_async_remote_copy(
                src_ref=branch_part.at[cb_peer(d)],
                dst_ref=branch_in.at[d - 1],
                send_sem=small_send.at[1],
                recv_sem=small_recv.at[1],
                device_id={"cb": cb_peer(d)},
                device_id_type=MESH,
            ).start()

        wait_bytes(squares_in, small_send.at[0])

        @pl.loop(0, chunks)
        def _(c):
            wait_bytes(part_in.at[c], part_send.at[c])
            wait_bytes(hid.at[c, pl.ds(0, nra - 1)], hid_send.at[c])

        wait_bytes(branch_in, small_recv.at[1])
        own = acc[pl.ds(pl.multiple_of(cb * crow, crow), crow), :]
        for d in range(1, ncb):
            own = own + branch_in[d - 1].astype(F32)
        branch[cb] = own.astype(BF16)
        for d in range(1, ncb):
            pltpu.make_async_remote_copy(
                src_ref=branch.at[cb],
                dst_ref=branch.at[cb],
                send_sem=small_send.at[2],
                recv_sem=small_recv.at[2],
                device_id={"cb": cb_peer(d)},
                device_id_type=MESH,
            ).start()
        wait_bytes(branch.at[pl.ds(0, ncb - 1)], small_recv.at[2])
        gathered = branch[...].reshape(tokens, depth).astype(F32)
        result = 0.5 * stream[...] + 0.5 * gathered * dscale_ref[...]
        if half == 0:
            stream[...] = result
        else:
            out_ref[...] = result
        wait_bytes(branch_in, small_send.at[1])
        wait_bytes(branch_in, small_send.at[2])


def local(nra, ncb, *args):
    (tokens, gain1, gate1, gscale1, up1, uscale1, down1, dscale1) = args[:8]
    (gain2, gate2, gscale2, up2, uscale2, down2, dscale2) = args[8:]
    count, depth = tokens.shape
    hidden = gate1.shape[1]
    size = chunk_of(hidden)
    chunks = hidden // size
    rows, crow = count // nra, count // ncb

    def row(vector):
        return vector.reshape(1, -1)

    vmem = pl.BlockSpec(memory_space=pltpu.VMEM)
    hbm = pl.BlockSpec(memory_space=pl.ANY)
    return pl.pallas_call(
        functools.partial(kernel, nra, ncb, float(depth * nra)),
        out_shape=jax.ShapeDtypeStruct((count, depth), F32),
        in_specs=[vmem] * 9 + [hbm] * 6,
        out_specs=vmem,
        scratch_shapes=[
            pltpu.VMEM((chunks, depth, size), F32),
            pltpu.VMEM((chunks, depth, size), F32),
            pltpu.VMEM((chunks, size, depth), F32),
            pltpu.VMEM((count, depth), F32),
            pltpu.VMEM((count, depth), BF16),
            pltpu.VMEM((count, depth), F32),
            pltpu.VMEM((nra, rows, 128), F32),
            pltpu.VMEM((nra - 1, rows, 128), F32),
            pltpu.VMEM((chunks, nra, rows, 2 * size), BF16),
            pltpu.VMEM((chunks, nra - 1, rows, 2 * size), BF16),
            pltpu.VMEM((chunks, nra, rows, size), BF16),
            pltpu.VMEM((ncb, crow, depth), BF16),
            pltpu.VMEM((ncb - 1, crow, depth), BF16),
            pltpu.VMEM((ncb, crow, depth), BF16),
            pltpu.SemaphoreType.DMA((chunks,)),
            pltpu.SemaphoreType.DMA((chunks,)),
            pltpu.SemaphoreType.DMA((chunks,)),
            pltpu.SemaphoreType.DMA((chunks,)),
            pltpu.SemaphoreType.DMA((chunks,)),
            pltpu.SemaphoreType.DMA((chunks,)),
            pltpu.SemaphoreType.DMA((chunks,)),
            pltpu.SemaphoreType.DMA((3,)),
            pltpu.SemaphoreType.DMA((3,)),
        ],
        compiler_params=pltpu.CompilerParams(
            collective_id=0, has_side_effects=True, vmem_limit_bytes=60 * 1024 * 1024
        ),
    )(
        tokens,
        row(gain1),
        row(gscale1),
        row(uscale1),
        row(dscale1),
        row(gain2),
        row(gscale2),
        row(uscale2),
        row(dscale2),
        gate1,
        up1,
        down1,
        gate2,
        up2,
        down2,
    )


def solution(mesh):
    half = (P("ra"), P("ra", "cb"), P("cb"), P("ra", "cb"), P("cb"), P("cb", "ra"), P("ra"))
    return jax.shard_map(
        functools.partial(local, mesh.shape["ra"], mesh.shape["cb"]),
        mesh=mesh,
        in_specs=(P("dp", "ra"),) + half + half,
        out_specs=P("dp", "ra"),
        check_vma=False,
    )
```

```python
import functools

import jax
import jax.numpy as jnp
from jax import lax
from jax.experimental import pallas as pl
from jax.experimental.pallas import tpu as pltpu
from jax.sharding import PartitionSpec as P

MESH = pl.DeviceIdType.MESH
F32 = jnp.float32
BF16 = jnp.bfloat16
REDUCE_LAG = 3
GATHER_LAG = 3


def chunk_of(total):
    for size in (256, 128):
        if total % size == 0:
            return size
    return total


def kernel(
    nra,
    ncb,
    width,
    tokens_ref,
    gain1_ref,
    gscale1_ref,
    uscale1_ref,
    dscale1_ref,
    gain2_ref,
    gscale2_ref,
    uscale2_ref,
    dscale2_ref,
    gate1_hbm,
    up1_hbm,
    down1_hbm,
    gate2_hbm,
    up2_hbm,
    down2_hbm,
    out_ref,
    wg,
    wu,
    wd,
    stream,
    scaled,
    acc,
    squares,
    squares_in,
    inverse_ref,
    part,
    part_out,
    part_in,
    hid,
    branch_part,
    branch_in,
    branch,
    wg_sem,
    wu_sem,
    wd_sem,
    part_send,
    part_recv,
    hid_send,
    hid_recv,
    squares_send,
    small_send,
    small_recv,
):
    ra = lax.axis_index("ra")
    cb = lax.axis_index("cb")
    chunks, depth, size = wg.shape
    tokens = stream.shape[0]
    rows = tokens // 2
    crow = tokens // ncb
    last = nra - 1

    def columns(c):
        return pl.ds(pl.multiple_of(c * size, size), size)

    def load_in(gate_hbm, up_hbm, c):
        return (
            pltpu.make_async_copy(gate_hbm.at[:, columns(c)], wg.at[c], wg_sem.at[c]),
            pltpu.make_async_copy(up_hbm.at[:, columns(c)], wu.at[c], wu_sem.at[c]),
        )

    def load_down(down_hbm, c):
        return pltpu.make_async_copy(down_hbm.at[columns(c), :], wd.at[c], wd_sem.at[c])

    def cb_peer(d):
        return lax.rem(cb + d, ncb)

    def wait_bytes(ref, sem):
        pltpu.make_async_copy(ref, ref, sem).wait()

    hops = (last - ra, ra)
    onward = (lax.rem(ra + nra - 1, nra), lax.rem(ra + 1, nra))
    back = (onward[1], onward[0])
    owner = (0, last)

    @pl.loop(0, chunks)
    def _(c):
        for copy in load_in(gate1_hbm, up1_hbm, c):
            copy.start()

    @pl.loop(0, chunks)
    def _(c):
        load_down(down1_hbm, c).start()

    barrier = pltpu.get_barrier_semaphore()
    for d in range(1, nra):
        peer = lax.rem(ra + d, nra)
        pl.semaphore_signal(barrier, inc=1, device_id={"ra": peer}, device_id_type=MESH)
    for d in range(1, ncb):
        pl.semaphore_signal(barrier, inc=1, device_id={"cb": cb_peer(d)}, device_id_type=MESH)

    stream[...] = tokens_ref[...].astype(F32)
    pl.semaphore_wait(barrier, nra + ncb - 2)

    halves = (
        (gain1_ref, gscale1_ref, uscale1_ref, dscale1_ref, gate1_hbm, up1_hbm, down1_hbm),
        (gain2_ref, gscale2_ref, uscale2_ref, dscale2_ref, gate2_hbm, up2_hbm, down2_hbm),
    )
    for half in range(2):
        gain_ref, gscale_ref, uscale_ref, dscale_ref, gate_hbm, up_hbm, down_hbm = halves[half]
        value = stream[...]
        scaled[...] = (value * gain_ref[...]).astype(BF16)
        sums = jnp.sum(value * value, axis=1, keepdims=True)
        squares[...] = jnp.broadcast_to(sums, (tokens, 128)).reshape(2, rows, 128)
        for f in range(2):
            @pl.when(hops[f] < last)
            def _(f=f):
                pltpu.make_async_remote_copy(
                    src_ref=squares.at[f],
                    dst_ref=squares_in.at[hops[f]],
                    send_sem=squares_send.at[f],
                    recv_sem=small_recv.at[0],
                    device_id={"ra": owner[f]},
                    device_id_type=MESH,
                ).start()

        acc[...] = jnp.zeros_like(acc)

        def reduce_step(f, c):
            send = pltpu.make_async_remote_copy(
                src_ref=part_out.at[f, c],
                dst_ref=part_in.at[f, c],
                send_sem=part_send.at[f, c],
                recv_sem=part_recv.at[f, c],
                device_id={"ra": onward[f]},
                device_id_type=MESH,
            )

            @pl.when(hops[f] == 0)
            def _():
                part_out[f, c] = part[c, f].astype(BF16)
                send.start()

            @pl.when(jnp.logical_and(hops[f] > 0, hops[f] < last))
            def _():
                wait_bytes(part_in.at[f, c], part_recv.at[f, c])
                part_out[f, c] = (part[c, f] + part_in[f, c].astype(F32)).astype(BF16)
                send.start()

            @pl.when(hops[f] == last)
            def _():
                @pl.when(c == 0)
                def _():
                    wait_bytes(squares_in, small_recv.at[0])
                    total = squares[f]
                    for d in range(last):
                        total = total + squares_in[d]
                    inverse_ref[...] = lax.rsqrt(total / width + 1e-06)

                wait_bytes(part_in.at[f, c], part_recv.at[f, c])
                both = part[c, f] + part_in[f, c].astype(F32)
                inverse = inverse_ref[:, :1]
                gate = both[:, :size] * inverse * gscale_ref[:, columns(c)]
                up = both[:, size:] * inverse * uscale_ref[:, columns(c)]
                hid[c, f] = (gate / (1.0 + jnp.exp(-gate)) * up).astype(BF16)
                forward(f, c).start()

        def forward(f, c):
            return pltpu.make_async_remote_copy(
                src_ref=hid.at[c, f],
                dst_ref=hid.at[c, f],
                send_sem=hid_send.at[f, c],
                recv_sem=hid_recv.at[f, c],
                device_id={"ra": back[f]},
                device_id_type=MESH,
            )

        def gather_step(f, c):
            @pl.when(hops[f] < last)
            def _():
                wait_bytes(hid.at[c, f], hid_recv.at[f, c])

                @pl.when(hops[f] > 0)
                def _():
                    forward(f, c).start()

        def at_lag(step, lag, act):
            c = step - lag

            @pl.when(jnp.logical_and(c >= 0, c < chunks))
            def _():
                act(c)

        @pl.loop(0, chunks + (REDUCE_LAG + GATHER_LAG) * last)
        def _(step):
            @pl.when(step < chunks)
            def _():
                c = step
                for copy in load_in(gate_hbm, up_hbm, c):
                    copy.wait()
                lhs = scaled[...]
                gate = jnp.dot(lhs, wg[c].astype(BF16), preferred_element_type=F32)
                up = jnp.dot(lhs, wu[c].astype(BF16), preferred_element_type=F32)
                part[c, :, :, :size] = gate.reshape(2, rows, size)
                part[c, :, :, size:] = up.reshape(2, rows, size)
                if half == 0:
                    for copy in load_in(gate2_hbm, up2_hbm, c):
                        copy.start()

            for f in range(2):
                at_lag(step, REDUCE_LAG * hops[f], functools.partial(reduce_step, f))
            for f in range(2):
                at_lag(
                    step,
                    REDUCE_LAG * last + GATHER_LAG * (last - hops[f]),
                    functools.partial(gather_step, f),
                )

            def down_step(c):
                load_down(down_hbm, c).wait()
                acc[...] += jnp.dot(
                    hid[c].reshape(tokens, size), wd[c].astype(BF16), preferred_element_type=F32
                )
                if half == 0:
                    load_down(down2_hbm, c).start()

            nearest = jnp.minimum(hops[0], hops[1])
            at_lag(step, REDUCE_LAG * last + GATHER_LAG * (last - nearest), down_step)

        branch_part[...] = acc[...].astype(BF16).reshape(branch_part.shape)
        for d in range(1, ncb):
            pltpu.make_async_remote_copy(
                src_ref=branch_part.at[cb_peer(d)],
                dst_ref=branch_in.at[d - 1],
                send_sem=small_send.at[1],
                recv_sem=small_recv.at[1],
                device_id={"cb": cb_peer(d)},
                device_id_type=MESH,
            ).start()

        for f in range(2):
            @pl.when(hops[f] < last)
            def _(f=f):
                wait_bytes(squares.at[f], squares_send.at[f])

                @pl.loop(0, chunks)
                def _(c):
                    wait_bytes(part_out.at[f, c], part_send.at[f, c])

            @pl.when(hops[f] > 0)
            def _(f=f):
                @pl.loop(0, chunks)
                def _(c):
                    wait_bytes(hid.at[c, f], hid_send.at[f, c])

        wait_bytes(branch_in, small_recv.at[1])
        own = acc[pl.ds(pl.multiple_of(cb * crow, crow), crow), :]
        for d in range(1, ncb):
            own = own + branch_in[d - 1].astype(F32)
        branch[cb] = own.astype(BF16)
        for d in range(1, ncb):
            pltpu.make_async_remote_copy(
                src_ref=branch.at[cb],
                dst_ref=branch.at[cb],
                send_sem=small_send.at[2],
                recv_sem=small_recv.at[2],
                device_id={"cb": cb_peer(d)},
                device_id_type=MESH,
            ).start()
        wait_bytes(branch.at[pl.ds(0, ncb - 1)], small_recv.at[2])
        gathered = branch[...].reshape(tokens, depth).astype(F32)
        result = 0.5 * stream[...] + 0.5 * gathered * dscale_ref[...]
        if half == 0:
            stream[...] = result
        else:
            out_ref[...] = result
        wait_bytes(branch_in, small_send.at[1])
        wait_bytes(branch_in, small_send.at[2])


def local(nra, ncb, *args):
    (tokens, gain1, gate1, gscale1, up1, uscale1, down1, dscale1) = args[:8]
    (gain2, gate2, gscale2, up2, uscale2, down2, dscale2) = args[8:]
    count, depth = tokens.shape
    hidden = gate1.shape[1]
    size = chunk_of(hidden)
    chunks = hidden // size
    rows, crow = count // 2, count // ncb

    def row(vector):
        return vector.reshape(1, -1)

    vmem = pl.BlockSpec(memory_space=pltpu.VMEM)
    hbm = pl.BlockSpec(memory_space=pl.ANY)
    return pl.pallas_call(
        functools.partial(kernel, nra, ncb, float(depth * nra)),
        out_shape=jax.ShapeDtypeStruct((count, depth), F32),
        in_specs=[vmem] * 9 + [hbm] * 6,
        out_specs=vmem,
        scratch_shapes=[
            pltpu.VMEM((chunks, depth, size), F32),
            pltpu.VMEM((chunks, depth, size), F32),
            pltpu.VMEM((chunks, size, depth), F32),
            pltpu.VMEM((count, depth), F32),
            pltpu.VMEM((count, depth), BF16),
            pltpu.VMEM((count, depth), F32),
            pltpu.VMEM((2, rows, 128), F32),
            pltpu.VMEM((nra - 1, rows, 128), F32),
            pltpu.VMEM((rows, 128), F32),
            pltpu.VMEM((chunks, 2, rows, 2 * size), F32),
            pltpu.VMEM((2, chunks, rows, 2 * size), BF16),
            pltpu.VMEM((2, chunks, rows, 2 * size), BF16),
            pltpu.VMEM((chunks, 2, rows, size), BF16),
            pltpu.VMEM((ncb, crow, depth), BF16),
            pltpu.VMEM((ncb - 1, crow, depth), BF16),
            pltpu.VMEM((ncb, crow, depth), BF16),
            pltpu.SemaphoreType.DMA((chunks,)),
            pltpu.SemaphoreType.DMA((chunks,)),
            pltpu.SemaphoreType.DMA((chunks,)),
            pltpu.SemaphoreType.DMA((2, chunks)),
            pltpu.SemaphoreType.DMA((2, chunks)),
            pltpu.SemaphoreType.DMA((2, chunks)),
            pltpu.SemaphoreType.DMA((2, chunks)),
            pltpu.SemaphoreType.DMA((2,)),
            pltpu.SemaphoreType.DMA((3,)),
            pltpu.SemaphoreType.DMA((3,)),
        ],
        compiler_params=pltpu.CompilerParams(
            collective_id=0, has_side_effects=True, vmem_limit_bytes=60 * 1024 * 1024
        ),
    )(
        tokens,
        row(gain1),
        row(gscale1),
        row(uscale1),
        row(dscale1),
        row(gain2),
        row(gscale2),
        row(uscale2),
        row(dscale2),
        gate1,
        up1,
        down1,
        gate2,
        up2,
        down2,
    )


def solution(mesh):
    half = (P("ra"), P("ra", "cb"), P("cb"), P("ra", "cb"), P("cb"), P("cb", "ra"), P("ra"))
    return jax.shard_map(
        functools.partial(local, mesh.shape["ra"], mesh.shape["cb"]),
        mesh=mesh,
        in_specs=(P("dp", "ra"),) + half + half,
        out_specs=P("dp", "ra"),
        check_vma=False,
    )
```
